32 devices in a mesh: sp: 16 (over z, y, x), tp: 2 (over core).
Axes of the slice: x: 2, y: 2, z: 4, core: 2. Of those that a mesh axis runs over, the one named last changes fastest.
Arguments:
- queries: bfloat16 [2048, 768], P('sp', 'tp'), may hold values from -6 to 6
- latents: bfloat16 [2048, 512], P('sp'), may hold values from -6 to 6
- rot_key: bfloat16 [2048, 32], P('sp'), may hold values from -6 to 6
- kv_weight: bfloat16 [512, 1024], P(None, 'tp'), may hold values from -0.25 to 0.25
- log_sums: float32 [2048, 8], P('sp', 'tp'), may hold values from 4 to 14, as said below
- outputs: bfloat16 [2048, 512], P('sp', 'tp'), may hold values from -4 to 4
- out_grad: bfloat16 [2048, 512], P('sp', 'tp'), may hold values from -96 to 96
Outputs:
- query_grad: bfloat16 [2048, 768], P('sp', 'tp')
- key_grad: bfloat16 [2048, 512], P('sp', 'tp')
- value_grad: bfloat16 [2048, 512], P('sp', 'tp')
- rot_grad: float32 [2048, 32], P('sp')
- weight_grad: float32 [512, 1024], P('sp', 'tp')
The draws below stay inside these ranges and needn't reach their ends.
Inputs may be any that keep to these rules, and one draw needn't show every extreme that they name: `log_sums`: each value lies within one half of log(2048) + 0.5.
All inputs are finite; a program needn't handle non-finite values.
Results may differ from the reference program's by a relative error of at most 0.004.
The reference program's roundings to bfloat16 on the way (of `joined`, `key_full`, `probs_b` and `dscore`) count: a program that leaves them out, or rounds other values in their place, can miss the bound.
Values may be sent and summed in bfloat16 or wider, within the bound.
A program may use at most 64 MiB of HBM per device.

```python
import math
import jax
import jax.numpy as jnp
from jax import lax

HEADS = 8
RANK = 512
NOPE_DIM = 64
ROPE_DIM = 32
VALUE_DIM = 64
SEQ = 2048


def draw_log_sums(key, part):
    center = math.log(SEQ) + 0.5
    return center + jax.random.uniform(key, (SEQ, HEADS), jnp.float32, -0.5, 0.5)


def with_spikes(result, own_key, source, target, parts, factor):
    def block_of(dim):
        return (jnp.arange(result.shape[dim]) // (result.shape[dim] // parts)).reshape((-1,) + (1,) * (result.ndim - 1 - dim))

    near = jax.random.permutation(own_key, parts)[block_of(target)]
    other_side = (block_of(target) + parts // 2) % parts
    return jnp.where((block_of(source) == near) | (block_of(source) == other_side), factor * result, result)


def block_scale(rng, dims, split, low, top_value):
    def one(dim, blocks):
        draws = jax.random.uniform(jax.random.fold_in(jax.random.fold_in(rng, 6), dim), (blocks,), jnp.float32, low / len(split), top_value / len(split))
        return jnp.repeat(jnp.exp(draws), dims[dim] // blocks).reshape((-1,) + (1,) * (len(dims) - dim - 1))

    loudness = one(*split[0])
    for cut in split[1:]:
        loudness = loudness * one(*cut)
    return loudness


def normal_values(key, shape, deviation, reach, shards=(), kind=jnp.bfloat16):
    array = jax.random.normal(key, shape, jnp.float32) * deviation
    if len(shards) > 0:
        array = block_scale(key, shape, shards, -0.22, 0.18) * array
    return jnp.clip(array, min=-reach, max=reach).astype(kind)


def noise_with(own_key, extent, spread, limit, pieces, heavy, held_as=jnp.bfloat16):
    entries = spread * jax.random.normal(own_key, extent, jnp.float32)
    if pieces:
        entries = entries * block_scale(own_key, extent, pieces, -0.22, 0.18)
    return jnp.clip(with_spikes(entries, jax.random.fold_in(own_key, 3), *heavy), -limit, limit).astype(held_as)


def setup_inputs(seed: int = 0) -> dict:
    splits = jax.random.split(jax.random.key(seed), 8)
    queries = normal_values(splits[0], (SEQ, HEADS * (NOPE_DIM + ROPE_DIM)), 1.0, 6.0, ((0, 16), (1, 2)))
    latents = normal_values(splits[1], (SEQ, RANK), 1.0, 6.0, ((0, 16),))
    rot_key = normal_values(splits[2], (SEQ, ROPE_DIM), 1.0, 6.0, ((0, 16),))
    kv_weight = normal_values(splits[3], (RANK, HEADS * (NOPE_DIM + VALUE_DIM)), RANK ** -0.5, 0.25, ((1, 2),))
    log_sums = draw_log_sums(jax.random.fold_in(splits[7], 71), 0)
    outputs = normal_values(splits[5], (SEQ, HEADS * VALUE_DIM), 0.3, 4.0, ((0, 16), (1, 2)))
    out_grad = noise_with(splits[6], (SEQ, HEADS * VALUE_DIM), (SEQ ** 0.5 / 4), 96.0, ((0, 16), (1, 2)), (0, 1, 16, 2.0))
    return dict(queries=queries, latents=latents, rot_key=rot_key, kv_weight=kv_weight, log_sums=log_sums, outputs=outputs, out_grad=out_grad)


def round_keep(values):
    rounded = values.astype(jnp.bfloat16)
    rounded = lax.optimization_barrier(rounded)
    return rounded.astype(jnp.float32)


def reference(queries, latents, rot_key, kv_weight, log_sums, outputs, out_grad):
    head_dim = NOPE_DIM + ROPE_DIM
    score_scale = head_dim ** -0.5
    joined = jnp.dot(latents, kv_weight, preferred_element_type=jnp.float32).astype(jnp.bfloat16)
    joined = joined.reshape(SEQ, HEADS, NOPE_DIM + VALUE_DIM).astype(jnp.float32)
    rotary = jnp.broadcast_to(rot_key.astype(jnp.float32)[:, None, :], (SEQ, HEADS, ROPE_DIM))
    key_full = jnp.concatenate([joined[:, :, :NOPE_DIM], rotary], axis=-1)
    values = joined[:, :, NOPE_DIM:]
    query_full = queries.astype(jnp.float32).reshape(SEQ, HEADS, head_dim)
    grad_full = out_grad.astype(jnp.float32).reshape(SEQ, HEADS, VALUE_DIM)
    row_delta = jnp.sum(outputs.astype(jnp.float32).reshape(SEQ, HEADS, VALUE_DIM) * grad_full, axis=-1)
    block_rows = math.gcd(SEQ, 512)
    block_count = SEQ // block_rows

    def block_step(totals, block_index):
        key_total, value_total = totals
        begin_row = (block_index * block_rows).astype(jnp.int32)
        query_block = lax.dynamic_slice_in_dim(query_full, begin_row, block_rows, 0)
        grad_block = lax.dynamic_slice_in_dim(grad_full, begin_row, block_rows, 0)
        log_block = lax.dynamic_slice_in_dim(log_sums, begin_row, block_rows, 0)
        delta_block = lax.dynamic_slice_in_dim(row_delta, begin_row, block_rows, 0)
        scores = jnp.einsum('qhd,khd->hqk', query_block, key_full) * score_scale
        probs = jnp.exp(scores - log_block.T[:, :, None])
        dprob = jnp.einsum('qhd,khd->hqk', grad_block, values)
        dscore = round_keep(probs * (dprob - delta_block.T[:, :, None]))
        probs_b = round_keep(probs)
        query_part = (jnp.einsum('hqk,khd->qhd', dscore, key_full) * score_scale).astype(jnp.bfloat16)
        key_total = key_total + jnp.einsum('hqk,qhd->khd', dscore, query_block) * score_scale
        value_total = value_total + jnp.einsum('hqk,qhd->khd', probs_b, grad_block)
        return (key_total, value_total), query_part

    start_totals = (jnp.zeros((SEQ, HEADS, head_dim), jnp.float32), jnp.zeros((SEQ, HEADS, VALUE_DIM), jnp.float32))
    (key_total, value_total), query_blocks = lax.scan(block_step, start_totals, jnp.arange(block_count, dtype=jnp.int32))
    query_grad = query_blocks.reshape(SEQ, HEADS * head_dim)
    rot_grad = jnp.sum(key_total[:, :, NOPE_DIM:], axis=1)
    key_grad = key_total[:, :, :NOPE_DIM].astype(jnp.bfloat16)
    value_grad = value_total.astype(jnp.bfloat16)
    stacked = jnp.concatenate([key_grad, value_grad], axis=-1).reshape(SEQ, HEADS * (NOPE_DIM + VALUE_DIM))
    weight_grad = jnp.dot(latents.T, stacked, preferred_element_type=jnp.float32)
    return (query_grad, key_grad.reshape(SEQ, HEADS * NOPE_DIM), value_grad.reshape(SEQ, HEADS * VALUE_DIM), rot_grad, weight_grad)
```

```python
import functools
import math

import jax
import jax.numpy as jnp
from jax import lax
from jax.experimental import pallas as pl
from jax.experimental.pallas import tpu as pltpu
from jax.sharding import PartitionSpec as P

NOPE = 64
ROPE = 32
VDIM = 64
HEAD = NOPE + ROPE
MESH = pl.DeviceIdType.MESH
F32 = jnp.float32
BF16 = jnp.bfloat16


def dot(x, y, dims):
    return lax.dot_general(x, y, (dims, ((), ())), preferred_element_type=F32)


def three_terms(x):
    hi = x.astype(BF16)
    rest = x - hi.astype(F32)
    mid = rest.astype(BF16)
    low = (rest - mid.astype(F32)).astype(BF16)
    return hi, mid, low


def repeat(start, stop, body):
    if stop - start <= 4:
        for i in range(start, stop):
            body(i)
    else:
        def step(i, carry):
            body(i)
            return carry

        lax.fori_loop(start, stop, step, 0)


def kernel(
    S, TP, H,
    q_ref, lat_ref, rot_ref, w_ref, log_ref, out_ref, go_ref,
    qg_ref, kg_ref, vg_ref, rg_ref, wg_ref,
    ps, pk, wq, kb, lb, ka_ref, va_ref, kat_ref, dk_acc, dv_acc, dq_own, dqs, dqr,
    kvo, kvr, ro, rr, rt, wgs, wgr, qo, qr,
    s1q, r1q, s1k, r1k, s1l, r1l, s2, r2, s3, r3, s4k, r4k, s4r, r4r, s4q, r4q, s5, r5, s6, r6,
):
    G = S // H
    T = q_ref.shape[0]
    half, quarter = T // 2, T // 4
    me = lax.axis_index("sp")
    tpi = lax.axis_index("tp")
    a, b = me // G, lax.rem(me, G)
    scale = HEAD ** (-0.5)

    barrier = pltpu.get_barrier_semaphore()

    def greet(i):
        pl.semaphore_signal(barrier, inc=1, device_id={"sp": lax.rem(me + i, S)}, device_id_type=MESH)

    def greet_tp(i):
        pl.semaphore_signal(barrier, inc=1, device_id={"tp": lax.rem(tpi + i, TP)}, device_id_type=MESH)

    repeat(1, S, greet)
    repeat(1, TP, greet_tp)

    def copy(src, dst, ssem, rsem, sp):
        return pltpu.make_async_remote_copy(
            src_ref=src, dst_ref=dst, send_sem=ssem, recv_sem=rsem,
            device_id={"sp": sp}, device_id_type=MESH,
        )

    prod = out_ref[...].astype(F32) * go_ref[...].astype(F32)
    pad = jnp.zeros((T, ROPE - 6), BF16)
    for j in range(H):
        delta = jnp.sum(prod[:, VDIM * j : VDIM * (j + 1)], axis=1, keepdims=True)
        logs = log_ref[:, j : j + 1] * math.sqrt(HEAD)
        terms = three_terms(logs) + three_terms(delta)
        ps[j, :T, :] = jnp.concatenate([q_ref[:, HEAD * j : HEAD * (j + 1)], *terms, pad], axis=1)
        g = go_ref[:, VDIM * j : VDIM * (j + 1)]
        ps[j, T:, :] = jnp.concatenate([g[:half], g[half:]], axis=1)
    joined = dot(lat_ref[...], w_ref[...], ((1,), (0,))).astype(BF16)
    rot = rot_ref[...]
    rot4 = jnp.concatenate([rot[quarter * i : quarter * (i + 1)] for i in range(4)], axis=1)
    for j in range(H):
        pk[j, :T, :] = joined[:, 128 * j : 128 * (j + 1)]
        pk[j, T:, :] = rot4
    wq[b, a] = ps[a]
    kb[a] = pk[a]
    lb[a] = lat_ref[...]
    pl.semaphore_wait(barrier, S - 1 + TP - 1)

    firsts, lats = [], []
    for d in range(1, H):
        to = lax.rem(a + d, H)
        cq = copy(ps.at[to], wq.at[b, a], s1q.at[d - 1], r1q.at[d - 1], to * G + b)
        ck = copy(pk.at[to], kb.at[a], s1k.at[d - 1], r1k.at[d - 1], to * G + b)
        cq.start()
        ck.start()
        firsts.append((cq, ck))

    def relay(d, e):
        src = wq.at[b, lax.rem(a - d + H, H)]
        return copy(src, src, s2.at[e - 1, d], r2.at[e - 1, d], a * G + lax.rem(b + e, G))

    def relay_all(d):
        repeat(1, G, lambda e: relay(d, e).start())

    relay_all(0)
    for d in range(1, H):
        to = lax.rem(a + d, H)
        cl = copy(lat_ref, lb.at[a], s1l.at[d - 1], r1l.at[d - 1], to * G + b)
        cl.start()
        lats.append(cl)
    for d in range(1, H):
        firsts[d - 1][0].wait_recv()
        relay_all(d)
    for d in range(1, H):
        firsts[d - 1][1].wait_recv()

    lane = lax.broadcasted_iota(jnp.int32, (T, ROPE), 1)
    log_ones = jnp.where(lane < 3, -1.0, 0.0).astype(BF16)
    delta_ones = jnp.where((lane >= 3) & (lane < 6), -1.0, 0.0).astype(BF16)
    for j in range(H):
        kv = kb[j, :T, :]
        r4 = kb[j, T:, :]
        r = jnp.concatenate([r4[:, ROPE * i : ROPE * (i + 1)] for i in range(4)], axis=0)
        key = jnp.concatenate([kv[:, :NOPE], r, log_ones], axis=1)
        ka_ref[T * j : T * (j + 1), :] = key
        va_ref[T * j : T * (j + 1), :128] = jnp.concatenate([jnp.zeros((T, HEAD), BF16), delta_ones], axis=1)
        va_ref[T * j : T * (j + 1), 128:] = jnp.concatenate([kv[:, NOPE:], jnp.zeros((T, 64), BF16)], axis=1)
        kat_ref[:, T * j : T * (j + 1)] = key.astype(F32).T.astype(BF16)[:HEAD]
    dk_acc[...] = jnp.zeros_like(dk_acc)
    dv_acc[...] = jnp.zeros_like(dv_acc)

    def block(e):
        col = lax.rem(b - e + G, G)
        query = wq[col, :, :T, :].reshape(H * T, 128)
        gp = wq[col, :, T:, :]
        g = jnp.concatenate([gp[:, :, :VDIM], gp[:, :, VDIM:]], axis=1).reshape(H * T, VDIM)
        g = jnp.concatenate([g, jnp.zeros_like(g)], axis=1)
        s = dot(ka_ref[...], query, ((1,), (1,)))
        dp = dot(va_ref[...], jnp.concatenate([query, g], axis=1), ((1,), (1,)))
        p = jnp.exp(s * scale)
        ds = (p * dp).astype(BF16)
        dv_acc[...] += dot(p.astype(BF16), g, ((1,), (0,)))
        dk_acc[...] += dot(ds, query, ((1,), (0,)))
        return dot(kat_ref[...], ds, ((1,), (0,))) * scale

    def part(e):
        return copy(dqs.at[e - 1], dqr.at[e - 1], s3.at[e - 1], r3.at[e - 1], a * G + lax.rem(b - e + G, G))

    dq_own[...] = block(0)

    def other(e):
        for d in range(H):
            relay(d, e).wait_recv()
        dqs[e - 1] = block(e)
        part(e).start()

    repeat(1, G, other)

    dk = dk_acc[...] * scale
    kv = jnp.concatenate([dk[:, :NOPE], dv_acc[:, :VDIM]], axis=1).astype(BF16)
    rot_t = dk.T[NOPE:HEAD]
    for j in range(H):
        kvo[j] = kv[T * j : T * (j + 1)]
        ro[j] = rot_t[:, T * j : T * (j + 1)]
    kvr[a] = kvo[a]
    rr[a] = ro[a]
    backs = []
    for d in range(1, H):
        to = lax.rem(a + d, H)
        ck = copy(kvo.at[to], kvr.at[a], s4k.at[d - 1], r4k.at[d - 1], to * G + b)
        cr = copy(ro.at[to], rr.at[a], s4r.at[d - 1], r4r.at[d - 1], to * G + b)
        cr.start()
        ck.start()
        backs += [ck, cr]

    for cl in lats:
        cl.wait_recv()
    total = None
    lat = lb[...].reshape(H * T, lb.shape[2])
    total = dot(lat, kv, ((0,), (0,)))
    wgs[...] = total.reshape(wgs.shape)
    wgr[me] = wgs[me]

    def share(i):
        to = lax.rem(me + i, S)
        return copy(wgs.at[to], wgr.at[me], s5.at[i - 1], r5.at[i - 1], to)

    repeat(1, S, lambda i: share(i).start())

    def take(e):
        part(e).wait_recv()
        dq_own[...] += dqr[e - 1]

    repeat(1, G, take)
    dq = jnp.concatenate([dq_own[...], jnp.zeros((128 - HEAD, H * T), F32)], axis=0).T.astype(BF16)
    for j in range(H):
        qo[j] = dq[T * j : T * (j + 1)]
    qr[a] = qo[a]
    for d in range(1, H):
        to = lax.rem(a + d, H)
        cq = copy(qo.at[to], qr.at[a], s4q.at[d - 1], r4q.at[d - 1], to * G + b)
        cq.start()
        backs.append(cq)

    for d in range(1, H):
        backs[2 * (d - 1) + 1].wait_recv()
    rt[tpi] = functools.reduce(lambda x, y: x + y, [rr[j] for j in range(H)])

    def swap(i):
        return pltpu.make_async_remote_copy(
            src_ref=rt.at[tpi], dst_ref=rt.at[tpi], send_sem=s6.at[i - 1], recv_sem=r6.at[i - 1],
            device_id={"tp": lax.rem(tpi + i, TP)}, device_id_type=MESH,
        )

    repeat(1, TP, lambda i: swap(i).start())
    for d in range(1, H):
        backs[2 * (d - 1)].wait_recv()
    for j in range(H):
        kg_ref[:, NOPE * j : NOPE * (j + 1)] = kvr[j, :, :NOPE]
        vg_ref[:, VDIM * j : VDIM * (j + 1)] = kvr[j, :, NOPE:]
    repeat(1, TP, lambda i: swap(i).wait_recv())
    rot_sum = functools.reduce(lambda x, y: x + y, [rt[i] for i in range(TP)])
    rg_ref[...] = jnp.concatenate([rot_sum, jnp.zeros((128 - ROPE, T), F32)], axis=0).T[:, :ROPE]
    repeat(1, S, lambda i: share(i).wait_recv())
    for j in range(H):
        wg_ref[:, 128 * j : 128 * (j + 1)] = functools.reduce(lambda x, y: x + y, [wgr[j * G + i] for i in range(G)])
    for d in range(1, H):
        backs[2 * (H - 1) + d - 1].wait_recv()
    for j in range(H):
        qg_ref[:, HEAD * j : HEAD * (j + 1)] = qr[j, :, :HEAD]

    for cq, ck in firsts:
        cq.wait_send()
        ck.wait_send()
    for c in lats + backs:
        c.wait_send()
    for d in range(H):
        repeat(1, G, lambda e: relay(d, e).wait_send())
    repeat(1, G, lambda e: part(e).wait_send())
    repeat(1, S, lambda i: share(i).wait_send())
    repeat(1, TP, lambda i: swap(i).wait_send())


def per_device(S, TP, queries, latents, rot_key, kv_weight, log_sums, outputs, out_grad):
    T, rank = latents.shape
    H = log_sums.shape[1]
    G = S // H
    rows = rank // S
    wide = H * T
    dma = lambda *n: pltpu.SemaphoreType.DMA(tuple(max(k, 1) for k in n))
    pairs = lambda *n: [dma(*n), dma(*n)]
    vm = pltpu.VMEM
    g1 = max(G - 1, 1)
    scratch = [
        vm((H, T + T // 2, 128), BF16), vm((H, T + T // 4, 128), BF16),
        vm((G, H, T + T // 2, 128), BF16), vm((H, T + T // 4, 128), BF16), vm((H, T, rank), BF16),
        vm((wide, 128), BF16), vm((wide, 256), BF16), vm((HEAD, wide), BF16),
        vm((wide, 128), F32), vm((wide, 128), F32), vm((HEAD, wide), F32),
        vm((g1, HEAD, wide), F32), vm((g1, HEAD, wide), F32),
        vm((H, T, 128), BF16), vm((H, T, 128), BF16), vm((H, ROPE, T), F32), vm((H, ROPE, T), F32),
        vm((TP, ROPE, T), F32), vm((S, rows, 128), F32), vm((S, rows, 128), F32),
        vm((H, T, 128), BF16), vm((H, T, 128), BF16),
        *pairs(H - 1), *pairs(H - 1), *pairs(H - 1), *pairs(G - 1, H), *pairs(G - 1),
        *pairs(H - 1), *pairs(H - 1), *pairs(H - 1), *pairs(S - 1), *pairs(TP - 1),
    ]
    return pl.pallas_call(
        functools.partial(kernel, S, TP, H),
        out_shape=[
            jax.ShapeDtypeStruct((T, H * HEAD), BF16),
            jax.ShapeDtypeStruct((T, H * NOPE), BF16),
            jax.ShapeDtypeStruct((T, H * VDIM), BF16),
            jax.ShapeDtypeStruct((T, ROPE), F32),
            jax.ShapeDtypeStruct((rows, H * 128), F32),
        ],
        in_specs=[pl.BlockSpec(memory_space=vm)] * 7,
        out_specs=[pl.BlockSpec(memory_space=vm)] * 5,
        scratch_shapes=scratch,
        compiler_params=pltpu.CompilerParams(
            collective_id=0, has_side_effects=True, vmem_limit_bytes=60000 * 1024
        ),
    )(queries, latents, rot_key, kv_weight, log_sums, outputs, out_grad)


def solution(mesh):
    placed = (
        P("sp", "tp"), P("sp", None), P("sp", None), P(None, "tp"),
        P("sp", "tp"), P("sp", "tp"), P("sp", "tp"),
    )
    return jax.shard_map(
        functools.partial(per_device, mesh.shape["sp"], mesh.shape["tp"]),
        mesh=mesh,
        in_specs=placed,
        out_specs=(P("sp", "tp"), P("sp", "tp"), P("sp", "tp"), P("sp", None), P("sp", "tp")),
        check_vma=False,
    )
```

```python
import functools
import math

import jax
import jax.numpy as jnp
from jax import lax
from jax.experimental import pallas as pl
from jax.experimental.pallas import tpu as pltpu
from jax.sharding import PartitionSpec as P

NOPE = 64
ROPE = 32
VDIM = 64
HEAD = NOPE + ROPE
MESH = pl.DeviceIdType.MESH
F32 = jnp.float32
BF16 = jnp.bfloat16


def dot(x, y, dims):
    return lax.dot_general(x, y, (dims, ((), ())), preferred_element_type=F32)


def three_terms(x):
    hi = x.astype(BF16)
    rest = x - hi.astype(F32)
    mid = rest.astype(BF16)
    low = (rest - mid.astype(F32)).astype(BF16)
    return hi, mid, low


def repeat(start, stop, body):
    if stop - start <= 4:
        for i in range(start, stop):
            body(i)
    else:
        def step(i, carry):
            body(i)
            return carry

        lax.fori_loop(start, stop, step, 0)


def kernel(
    S, TP, H,
    q_in, lat_in, rot_in, w_in, log_in, out_in, go_in,
    qg_ref, kg_ref, vg_ref, rg_ref, wg_ref,
    q_ref, lat_ref, rot_ref, w_ref, log_ref, out_ref, go_ref, loads, ps, pk, wq, kb, lb, ka_ref, va_ref, kat_ref, dk_acc, dv_acc, dq_own, dqs, dqr,
    kvo, kvr, ro, rr, rt, wgs, wgr, qo, qr,
    s1q, r1q, s1k, r1k, s1l, r1l, s2, r2, s3, r3, s4k, r4k, s4r, r4r, s4q, r4q, s5, r5, s6, r6,
):
    G = S // H
    T = q_ref.shape[0]
    half = T // 2
    me = lax.axis_index("sp")
    tpi = lax.axis_index("tp")
    a, b = me // G, lax.rem(me, G)
    scale = HEAD ** (-0.5)

    barrier = pltpu.get_barrier_semaphore()

    def greet(i):
        pl.semaphore_signal(barrier, inc=1, device_id={"sp": lax.rem(me + i, S)}, device_id_type=MESH)

    def greet_tp(i):
        pl.semaphore_signal(barrier, inc=1, device_id={"tp": lax.rem(tpi + i, TP)}, device_id_type=MESH)

    pairs = (
        (q_in, q_ref), (go_in, go_ref), (out_in, out_ref), (log_in, log_ref),
        (lat_in, lat_ref), (w_in, w_ref), (rot_in, rot_ref),
    )
    fetch = [pltpu.make_async_copy(x, y, loads.at[i]) for i, (x, y) in enumerate(pairs)]
    for f in fetch:
        f.start()
    repeat(1, S, greet)
    repeat(1, TP, greet_tp)

    def copy(src, dst, ssem, rsem, sp):
        return pltpu.make_async_remote_copy(
            src_ref=src, dst_ref=dst, send_sem=ssem, recv_sem=rsem,
            device_id={"sp": sp}, device_id_type=MESH,
        )

    for f in fetch[:4]:
        f.wait()
    logs_t = log_ref[...] * math.sqrt(HEAD)
    prod = out_ref[...].astype(F32) * go_ref[...].astype(F32)
    pad = jnp.zeros((T, ROPE - 6), BF16)
    for j in range(H):
        delta = jnp.sum(prod[:, VDIM * j : VDIM * (j + 1)], axis=1, keepdims=True)
        logs = jnp.broadcast_to(logs_t[j : j + 1], (8, T)).T[:, :1]
        terms = three_terms(logs) + three_terms(delta)
        ps[j, :T, :] = jnp.concatenate([q_ref[:, HEAD * j : HEAD * (j + 1)], *terms, pad], axis=1)
        g = go_ref[:, VDIM * j : VDIM * (j + 1)]
        ps[j, T:, :] = jnp.concatenate([g[:half], g[half:]], axis=1)
    wq[b, a] = ps[a]
    pl.semaphore_wait(barrier, S - 1 + TP - 1)

    firsts, lats = [], []
    for d in range(1, H):
        to = lax.rem(a + d, H)
        cq = copy(ps.at[to], wq.at[b, a], s1q.at[d - 1], r1q.at[d - 1], to * G + b)
        ck = copy(pk.at[to], kb.at[a], s1k.at[d - 1], r1k.at[d - 1], to * G + b)
        cq.start()
        firsts.append((cq, ck))

    def relay(d, e):
        src = wq.at[b, lax.rem(a - d + H, H)]
        return copy(src, src, s2.at[e - 1, d], r2.at[e - 1, d], a * G + lax.rem(b + e, G))

    def relay_all(d):
        repeat(1, G, lambda e: relay(d, e).start())

    relay_all(0)
    for f in fetch[4:]:
        f.wait()
    joined = dot(lat_ref[...], w_ref[...], ((1,), (0,))).astype(BF16)
    for j in range(H):
        pk[j, :T, :] = joined[:, 128 * j : 128 * (j + 1)]
        pk[j, T:, :] = rot_ref[...]
    kb[a] = pk[a]
    for d in range(1, H):
        firsts[d - 1][1].start()
    lb[a] = lat_ref[...]
    for d in range(1, H):
        to = lax.rem(a + d, H)
        cl = copy(lat_ref, lb.at[a], s1l.at[d - 1], r1l.at[d - 1], to * G + b)
        cl.start()
        lats.append(cl)
    for d in range(1, H):
        firsts[d - 1][0].wait_recv()
        relay_all(d)
    for d in range(1, H):
        firsts[d - 1][1].wait_recv()

    lane = lax.broadcasted_iota(jnp.int32, (T, ROPE), 1)
    log_ones = jnp.where(lane < 3, -1.0, 0.0).astype(BF16)
    delta_ones = jnp.where((lane >= 3) & (lane < 6), -1.0, 0.0).astype(BF16)
    for j in range(H):
        kv = kb[j, :T, :]
        r = kb[j, T:, :].astype(F32).T.astype(BF16)
        key = jnp.concatenate([kv[:, :NOPE], r, log_ones], axis=1)
        ka_ref[T * j : T * (j + 1), :] = key
        va_ref[T * j : T * (j + 1), :128] = jnp.concatenate([jnp.zeros((T, HEAD), BF16), delta_ones], axis=1)
        va_ref[T * j : T * (j + 1), 128:] = jnp.concatenate([kv[:, NOPE:], jnp.zeros((T, 64), BF16)], axis=1)
        kat_ref[:, T * j : T * (j + 1)] = key.astype(F32).T.astype(BF16)[:HEAD]
    dk_acc[...] = jnp.zeros_like(dk_acc)
    dv_acc[...] = jnp.zeros_like(dv_acc)

    def block(e):
        col = lax.rem(b - e + G, G)
        query = wq[col, :, :T, :].reshape(H * T, 128)
        gp = wq[col, :, T:, :]
        g = jnp.concatenate([gp[:, :, :VDIM], gp[:, :, VDIM:]], axis=1).reshape(H * T, VDIM)
        g = jnp.concatenate([g, jnp.zeros_like(g)], axis=1)
        s = dot(ka_ref[...], query, ((1,), (1,)))
        dp = dot(va_ref[...], jnp.concatenate([query, g], axis=1), ((1,), (1,)))
        p = jnp.exp(s * scale)
        ds = (p * dp).astype(BF16)
        dv_acc[...] += dot(p.astype(BF16), g, ((1,), (0,)))
        dk_acc[...] += dot(ds, query, ((1,), (0,)))
        return dot(kat_ref[...], ds, ((1,), (0,))) * scale

    def part(e):
        return copy(dqs.at[e - 1], dqr.at[e - 1], s3.at[e - 1], r3.at[e - 1], a * G + lax.rem(b - e + G, G))

    dq_own[...] = block(0)

    def other(e):
        for d in range(H):
            relay(d, e).wait_recv()
        dqs[e - 1] = block(e)
        part(e).start()

    repeat(1, G, other)

    dk = dk_acc[...] * scale
    kv = jnp.concatenate([dk[:, :NOPE], dv_acc[:, :VDIM]], axis=1).astype(BF16)
    rot_t = dk.T[NOPE:HEAD]
    for j in range(H):
        kvo[j] = kv[T * j : T * (j + 1)]
        ro[j] = rot_t[:, T * j : T * (j + 1)]
    kvr[a] = kvo[a]
    rr[a] = ro[a]
    backs = []
    for d in range(1, H):
        to = lax.rem(a + d, H)
        ck = copy(kvo.at[to], kvr.at[a], s4k.at[d - 1], r4k.at[d - 1], to * G + b)
        cr = copy(ro.at[to], rr.at[a], s4r.at[d - 1], r4r.at[d - 1], to * G + b)
        cr.start()
        ck.start()
        backs += [ck, cr]

    for cl in lats:
        cl.wait_recv()
    total = None
    lat = lb[...].reshape(H * T, lb.shape[2])
    total = dot(lat, kv, ((0,), (0,)))
    wgs[...] = total.reshape(wgs.shape)
    wgr[me] = wgs[me]

    def share(i):
        to = lax.rem(me + i, S)
        return copy(wgs.at[to], wgr.at[me], s5.at[i - 1], r5.at[i - 1], to)

    repeat(1, S, lambda i: share(i).start())

    def take(e):
        part(e).wait_recv()
        dq_own[...] += dqr[e - 1]

    repeat(1, G, take)
    dq = jnp.concatenate([dq_own[...], jnp.zeros((128 - HEAD, H * T), F32)], axis=0).T.astype(BF16)
    for j in range(H):
        qo[j] = dq[T * j : T * (j + 1)]
    qr[a] = qo[a]
    for d in range(1, H):
        to = lax.rem(a + d, H)
        cq = copy(qo.at[to], qr.at[a], s4q.at[d - 1], r4q.at[d - 1], to * G + b)
        cq.start()
        backs.append(cq)

    for d in range(1, H):
        backs[2 * (d - 1) + 1].wait_recv()
    rt[tpi] = functools.reduce(lambda x, y: x + y, [rr[j] for j in range(H)])

    def swap(i):
        return pltpu.make_async_remote_copy(
            src_ref=rt.at[tpi], dst_ref=rt.at[tpi], send_sem=s6.at[i - 1], recv_sem=r6.at[i - 1],
            device_id={"tp": lax.rem(tpi + i, TP)}, device_id_type=MESH,
        )

    repeat(1, TP, lambda i: swap(i).start())
    for d in range(1, H):
        backs[2 * (d - 1)].wait_recv()
    for j in range(H):
        kg_ref[:, NOPE * j : NOPE * (j + 1)] = kvr[j, :, :NOPE]
        vg_ref[:, VDIM * j : VDIM * (j + 1)] = kvr[j, :, NOPE:]
    repeat(1, TP, lambda i: swap(i).wait_recv())
    rot_sum = functools.reduce(lambda x, y: x + y, [rt[i] for i in range(TP)])
    rg_ref[...] = rot_sum
    repeat(1, S, lambda i: share(i).wait_recv())
    for j in range(H):
        wg_ref[:, 128 * j : 128 * (j + 1)] = functools.reduce(lambda x, y: x + y, [wgr[j * G + i] for i in range(G)])
    for d in range(1, H):
        backs[2 * (H - 1) + d - 1].wait_recv()
    for j in range(H):
        qg_ref[:, HEAD * j : HEAD * (j + 1)] = qr[j, :, :HEAD]

    for cq, ck in firsts:
        cq.wait_send()
        ck.wait_send()
    for c in lats + backs:
        c.wait_send()
    for d in range(H):
        repeat(1, G, lambda e: relay(d, e).wait_send())
    repeat(1, G, lambda e: part(e).wait_send())
    repeat(1, S, lambda i: share(i).wait_send())
    repeat(1, TP, lambda i: swap(i).wait_send())


def put_out(*refs):
    copies = [pltpu.make_async_copy(refs[i], refs[5 + i], refs[10].at[i]) for i in range(5)]
    for c in copies:
        c.start()
    for c in copies:
        c.wait()


def per_device(S, TP, queries, latents, rot_key, kv_weight, log_sums, outputs, out_grad):
    T, rank = latents.shape
    H = log_sums.shape[1]
    G = S // H
    rows = rank // S
    wide = H * T
    dma = lambda *n: pltpu.SemaphoreType.DMA(tuple(max(k, 1) for k in n))
    pairs = lambda *n: [dma(*n), dma(*n)]
    vm = pltpu.VMEM
    g1 = max(G - 1, 1)
    arrays = (queries, latents, rot_key.T, kv_weight, log_sums.T, outputs, out_grad)
    scratch = [
        *[vm(x.shape, x.dtype) for x in arrays], dma(len(arrays)),
        vm((H, T + T // 2, 128), BF16), vm((H, T + ROPE, 128), BF16),
        vm((G, H, T + T // 2, 128), BF16), vm((H, T + ROPE, 128), BF16), vm((H, T, rank), BF16),
        vm((wide, 128), BF16), vm((wide, 256), BF16), vm((HEAD, wide), BF16),
        vm((wide, 128), F32), vm((wide, 128), F32), vm((HEAD, wide), F32),
        vm((g1, HEAD, wide), F32), vm((g1, HEAD, wide), F32),
        vm((H, T, 128), BF16), vm((H, T, 128), BF16), vm((H, ROPE, T), F32), vm((H, ROPE, T), F32),
        vm((TP, ROPE, T), F32), vm((S, rows, 128), F32), vm((S, rows, 128), F32),
        vm((H, T, 128), BF16), vm((H, T, 128), BF16),
        *pairs(H - 1), *pairs(H - 1), *pairs(H - 1), *pairs(G - 1, H), *pairs(G - 1),
        *pairs(H - 1), *pairs(H - 1), *pairs(H - 1), *pairs(S - 1), *pairs(TP - 1),
    ]
    shapes = [
        ((T, H * HEAD), BF16), ((T, H * NOPE), BF16), ((T, H * VDIM), BF16),
        ((ROPE, T), F32), ((rows, H * 128), F32),
    ]
    results = pl.pallas_call(
        functools.partial(kernel, S, TP, H),
        out_shape=[pltpu.VMEM(*x) for x in shapes],
        in_specs=[pl.BlockSpec(memory_space=pltpu.HBM)] * 7,
        out_specs=[pl.BlockSpec(memory_space=vm)] * 5,
        scratch_shapes=scratch,
        compiler_params=pltpu.CompilerParams(
            collective_id=0, has_side_effects=True, vmem_limit_bytes=50000 * 1024
        ),
    )(*arrays)
    query_grad, key_grad, value_grad, rot_grad, weight_grad = pl.pallas_call(
        put_out,
        out_shape=[jax.ShapeDtypeStruct(*x) for x in shapes],
        in_specs=[pl.BlockSpec(memory_space=vm)] * 5,
        out_specs=[pl.BlockSpec(memory_space=pltpu.HBM)] * 5,
        scratch_shapes=[dma(5)],
    )(*results)
    return query_grad, key_grad, value_grad, rot_grad.T, weight_grad


def solution(mesh):
    placed = (
        P("sp", "tp"), P("sp", None), P("sp", None), P(None, "tp"),
        P("sp", "tp"), P("sp", "tp"), P("sp", "tp"),
    )
    return jax.shard_map(
        functools.partial(per_device, mesh.shape["sp"], mesh.shape["tp"]),
        mesh=mesh,
        in_specs=placed,
        out_specs=(P("sp", "tp"), P("sp", "tp"), P("sp", "tp"), P("sp", None), P("sp", "tp")),
        check_vma=False,
    )
```

```python
import functools
import math

import jax
import jax.numpy as jnp
from jax import lax
from jax.experimental import pallas as pl
from jax.experimental.pallas import tpu as pltpu
from jax.sharding import PartitionSpec as P

NOPE = 64
ROPE = 32
VDIM = 64
HEAD = NOPE + ROPE
VMEM_BYTES = 67043328
SPARE = 8192
MESH = pl.DeviceIdType.MESH
F32 = jnp.float32
BF16 = jnp.bfloat16


def dot(x, y, dims):
    return lax.dot_general(x, y, (dims, ((), ())), preferred_element_type=F32)


def three_terms(x):
    hi = x.astype(BF16)
    rest = x - hi.astype(F32)
    mid = rest.astype(BF16)
    low = (rest - mid.astype(F32)).astype(BF16)
    return hi, mid, low


def repeat(start, stop, body):
    if stop - start <= 4:
        for i in range(start, stop):
            body(i)
    else:
        def step(i, carry):
            body(i)
            return carry

        lax.fori_loop(start, stop, step, 0)


def kernel(
    S, TP, H,
    q_in, lat_in, rot_in, w_in, log_in, out_in, go_in,
    qg_ref, kg_ref, vg_ref, rg_ref, wg_ref,
    q_ref, lat_ref, rot_ref, w_ref, log_ref, out_ref, go_ref, loads, ps, pk, wq, kb, lb, ka_ref, va_ref, kat_ref, dk_acc, dv_acc, dq_own, dqs, dqr,
    kvo, kvr, ro, rr, rt, wgs, wgr, wh, wo, qo, qr,
    s1q, r1q, s1k, r1k, s1l, r1l, s2, r2, s3, r3, s4k, r4k, s4r, r4r, s4q, r4q, s5, r5, s6, r6, s7, r7,
):
    G = S // H
    T = q_ref.shape[0]
    half = T // 2
    me = lax.axis_index("sp")
    tpi = lax.axis_index("tp")
    a, b = me // G, lax.rem(me, G)
    scale = HEAD ** (-0.5)

    barrier = pltpu.get_barrier_semaphore()

    def greet(i):
        pl.semaphore_signal(barrier, inc=1, device_id={"sp": lax.rem(me + i, S)}, device_id_type=MESH)

    def greet_tp(i):
        pl.semaphore_signal(barrier, inc=1, device_id={"tp": lax.rem(tpi + i, TP)}, device_id_type=MESH)

    pairs = (
        (q_in, q_ref), (go_in, go_ref), (out_in, out_ref), (log_in, log_ref),
        (lat_in, lat_ref), (w_in, w_ref), (rot_in, rot_ref),
    )
    fetch = [pltpu.make_async_copy(x, y, loads.at[i]) for i, (x, y) in enumerate(pairs)]
    for f in fetch:
        f.start()
    repeat(1, S, greet)
    repeat(1, TP, greet_tp)

    def copy(src, dst, ssem, rsem, sp):
        return pltpu.make_async_remote_copy(
            src_ref=src, dst_ref=dst, send_sem=ssem, recv_sem=rsem,
            device_id={"sp": sp}, device_id_type=MESH,
        )

    for f in fetch[:4]:
        f.wait()
    logs_t = log_ref[...] * math.sqrt(HEAD)
    prod = out_ref[...].astype(F32) * go_ref[...].astype(F32)
    pad = jnp.zeros((T, ROPE - 6), BF16)
    for j in range(H):
        delta = jnp.sum(prod[:, VDIM * j : VDIM * (j + 1)], axis=1, keepdims=True)
        logs = jnp.broadcast_to(logs_t[j : j + 1], (8, T)).T[:, :1]
        terms = three_terms(logs) + three_terms(delta)
        ps[j, :T, :] = jnp.concatenate([q_ref[:, HEAD * j : HEAD * (j + 1)], *terms, pad], axis=1)
        g = go_ref[:, VDIM * j : VDIM * (j + 1)]
        ps[j, T:, :] = jnp.concatenate([g[:half], g[half:]], axis=1)
    wq[b, a] = ps[a]
    pl.semaphore_wait(barrier, S - 1 + TP - 1)

    firsts, lats = [], []
    for d in range(1, H):
        to = lax.rem(a + d, H)
        cq = copy(ps.at[to], wq.at[b, a], s1q.at[d - 1], r1q.at[d - 1], to * G + b)
        ck = copy(pk.at[to], kb.at[a], s1k.at[d - 1], r1k.at[d - 1], to * G + b)
        cq.start()
        firsts.append((cq, ck))

    def relay(d, e):
        src = wq.at[b, lax.rem(a - d + H, H)]
        return copy(src, src, s2.at[e - 1, d], r2.at[e - 1, d], a * G + lax.rem(b + e, G))

    def relay_all(d):
        repeat(1, G, lambda e: relay(d, e).start())

    relay_all(0)
    for f in fetch[4:]:
        f.wait()
    joined = dot(lat_ref[...], w_ref[...], ((1,), (0,))).astype(BF16)
    for j in range(H):
        pk[j, :T, :] = joined[:, 128 * j : 128 * (j + 1)]
        pk[j, T:, :] = rot_ref[...]
    kb[a] = pk[a]
    for d in range(1, H):
        firsts[d - 1][1].start()
    lb[a] = lat_ref[...]
    for d in range(1, H):
        to = lax.rem(a + d, H)
        cl = copy(lat_ref, lb.at[a], s1l.at[d - 1], r1l.at[d - 1], to * G + b)
        cl.start()
        lats.append(cl)
    for d in range(1, H):
        firsts[d - 1][0].wait_recv()
        relay_all(d)
    for d in range(1, H):
        firsts[d - 1][1].wait_recv()

    lane = lax.broadcasted_iota(jnp.int32, (T, ROPE), 1)
    log_ones = jnp.where(lane < 3, -1.0, 0.0).astype(BF16)
    delta_ones = jnp.where((lane >= 3) & (lane < 6), -1.0, 0.0).astype(BF16)
    for j in range(H):
        kv = kb[j, :T, :]
        r = kb[j, T:, :].astype(F32).T.astype(BF16)
        key = jnp.concatenate([kv[:, :NOPE], r, log_ones], axis=1)
        ka_ref[T * j : T * (j + 1), :] = key
        va_ref[T * j : T * (j + 1), :128] = jnp.concatenate([jnp.zeros((T, HEAD), BF16), delta_ones], axis=1)
        va_ref[T * j : T * (j + 1), 128:] = jnp.concatenate([kv[:, NOPE:], jnp.zeros((T, 64), BF16)], axis=1)
        kat_ref[:, T * j : T * (j + 1)] = key.astype(F32).T.astype(BF16)[:HEAD]
    dk_acc[...] = jnp.zeros_like(dk_acc)
    dv_acc[...] = jnp.zeros_like(dv_acc)

    def block(e, keep):
        col = lax.rem(b - e + G, G)
        query = wq[col, :, :T, :].reshape(H * T, 128)
        gp = wq[col, :, T:, :]
        g = jnp.concatenate([gp[:, :, :VDIM], gp[:, :, VDIM:]], axis=1).reshape(H * T, VDIM)
        g = jnp.concatenate([g, jnp.zeros_like(g)], axis=1)
        s = dot(ka_ref[...], query, ((1,), (1,)))
        dp = dot(va_ref[...], jnp.concatenate([query, g], axis=1), ((1,), (1,)))
        p = jnp.exp(s * scale)
        ds = (p * dp).astype(BF16)
        keep(dot(kat_ref[...], ds, ((1,), (0,))) * scale)
        dv_acc[...] += dot(p.astype(BF16), g, ((1,), (0,)))
        dk_acc[...] += dot(ds, query, ((1,), (0,)))

    def part(e):
        return copy(dqs.at[e - 1], dqr.at[e - 1], s3.at[e - 1], r3.at[e - 1], a * G + lax.rem(b - e + G, G))

    def keep_own(x):
        dq_own[...] = x

    block(0, keep_own)

    def other(e):
        for d in range(H):
            relay(d, e).wait_recv()

        def send(x):
            dqs[e - 1] = x
            part(e).start()

        block(e, send)

    repeat(1, G, other)

    dk = dk_acc[...] * scale
    kv = jnp.concatenate([dk[:, :NOPE], dv_acc[:, :VDIM]], axis=1).astype(BF16)
    rot_t = dk.T[NOPE:HEAD]
    for j in range(H):
        kvo[j] = kv[T * j : T * (j + 1)]
        ro[j] = rot_t[:, T * j : T * (j + 1)]
    kvr[a] = kvo[a]
    rr[a] = ro[a]
    backs = []
    for d in range(1, H):
        to = lax.rem(a + d, H)
        ck = copy(kvo.at[to], kvr.at[a], s4k.at[d - 1], r4k.at[d - 1], to * G + b)
        cr = copy(ro.at[to], rr.at[a], s4r.at[d - 1], r4r.at[d - 1], to * G + b)
        cr.start()
        ck.start()
        backs += [ck, cr]

    for cl in lats:
        cl.wait_recv()
    lat = lb[...].reshape(H * T, lb.shape[2])
    total = dot(lat, kv, ((0,), (0,)))
    rows = wgs.shape[2]
    for i in range(G):
        for j in range(H):
            wgs[i, j] = total[(j * G + i) * rows : (j * G + i + 1) * rows]
    wgr[b] = wgs[b]

    def share(e):
        to = lax.rem(b + e, G)
        return copy(wgs.at[to], wgr.at[b], s5.at[e - 1], r5.at[e - 1], a * G + to)

    repeat(1, G, lambda e: share(e).start())

    def take(e):
        part(e).wait_recv()
        dq_own[...] += dqr[e - 1]

    repeat(1, G, take)
    dq = jnp.concatenate([dq_own[...], jnp.zeros((128 - HEAD, H * T), F32)], axis=0).T.astype(BF16)
    for j in range(H):
        qo[j] = dq[T * j : T * (j + 1)]
    qr[a] = qo[a]
    for d in range(1, H):
        to = lax.rem(a + d, H)
        cq = copy(qo.at[to], qr.at[a], s4q.at[d - 1], r4q.at[d - 1], to * G + b)
        cq.start()
        backs.append(cq)

    repeat(1, G, lambda e: share(e).wait_recv())
    wh[...] = functools.reduce(lambda x, y: x + y, [wgr[i] for i in range(G)])
    wo[a] = wh[a]
    lasts = []
    for d in range(1, H):
        to = lax.rem(a + d, H)
        c = copy(wh.at[to], wo.at[a], s7.at[d - 1], r7.at[d - 1], to * G + b)
        c.start()
        lasts.append(c)
    for d in range(1, H):
        backs[2 * (d - 1) + 1].wait_recv()
    rt[tpi] = functools.reduce(lambda x, y: x + y, [rr[j] for j in range(H)])

    def swap(i):
        return pltpu.make_async_remote_copy(
            src_ref=rt.at[tpi], dst_ref=rt.at[tpi], send_sem=s6.at[i - 1], recv_sem=r6.at[i - 1],
            device_id={"tp": lax.rem(tpi + i, TP)}, device_id_type=MESH,
        )

    repeat(1, TP, lambda i: swap(i).start())
    for d in range(1, H):
        backs[2 * (d - 1)].wait_recv()
    for j in range(H):
        kg_ref[:, NOPE * j : NOPE * (j + 1)] = kvr[j, :, :NOPE]
        vg_ref[:, VDIM * j : VDIM * (j + 1)] = kvr[j, :, NOPE:]
    repeat(1, TP, lambda i: swap(i).wait_recv())
    rot_sum = functools.reduce(lambda x, y: x + y, [rt[i] for i in range(TP)])
    rg_ref[...] = rot_sum
    for d in range(1, H):
        backs[2 * (H - 1) + d - 1].wait_recv()
    for j in range(H):
        qg_ref[:, HEAD * j : HEAD * (j + 1)] = qr[j, :, :HEAD]

    for c in lasts:
        c.wait_recv()
    for j in range(H):
        wg_ref[:, 128 * j : 128 * (j + 1)] = wo[j]

    for cq, ck in firsts:
        cq.wait_send()
        ck.wait_send()
    for c in lats + backs + lasts:
        c.wait_send()
    for d in range(H):
        repeat(1, G, lambda e: relay(d, e).wait_send())
    repeat(1, G, lambda e: part(e).wait_send())
    repeat(1, G, lambda e: share(e).wait_send())
    repeat(1, TP, lambda i: swap(i).wait_send())


def put_out(*refs):
    copies = [pltpu.make_async_copy(refs[i], refs[5 + i], refs[10].at[i]) for i in range(5)]
    for c in copies:
        c.start()
    for c in copies:
        c.wait()


def per_device(S, TP, queries, latents, rot_key, kv_weight, log_sums, outputs, out_grad):
    T, rank = latents.shape
    H = log_sums.shape[1]
    G = S // H
    rows = rank // S
    wide = H * T
    dma = lambda *n: pltpu.SemaphoreType.DMA(tuple(max(k, 1) for k in n))
    pairs = lambda *n: [dma(*n), dma(*n)]
    vm = pltpu.VMEM
    g1 = max(G - 1, 1)
    arrays = (queries, latents, rot_key.T, kv_weight, log_sums.T, outputs, out_grad)
    scratch = [
        *[vm(x.shape, x.dtype) for x in arrays], dma(len(arrays)),
        vm((H, T + T // 2, 128), BF16), vm((H, T + ROPE, 128), BF16),
        vm((G, H, T + T // 2, 128), BF16), vm((H, T + ROPE, 128), BF16), vm((H, T, rank), BF16),
        vm((wide, 128), BF16), vm((wide, 256), BF16), vm((HEAD, wide), BF16),
        vm((wide, 128), F32), vm((wide, 128), F32), vm((HEAD, wide), F32),
        vm((g1, HEAD, wide), F32), vm((g1, HEAD, wide), F32),
        vm((H, T, 128), BF16), vm((H, T, 128), BF16), vm((H, ROPE, T), F32), vm((H, ROPE, T), F32),
        vm((TP, ROPE, T), F32), *[vm((G, H, rows, 128), F32)] * 2, *[vm((H, rows, 128), F32)] * 2,
        vm((H, T, 128), BF16), vm((H, T, 128), BF16),
        *pairs(H - 1), *pairs(H - 1), *pairs(H - 1), *pairs(G - 1, H), *pairs(G - 1),
        *pairs(H - 1), *pairs(H - 1), *pairs(H - 1), *pairs(G - 1), *pairs(TP - 1), *pairs(H - 1),
    ]
    shapes = [
        ((T, H * HEAD), BF16), ((T, H * NOPE), BF16), ((T, H * VDIM), BF16),
        ((ROPE, T), F32), ((rows, H * 128), F32),
    ]
    held = sum(x[0] * -(-x[1] // 128) * 128 * jnp.dtype(t).itemsize for x, t in shapes)
    results = pl.pallas_call(
        functools.partial(kernel, S, TP, H),
        out_shape=[pltpu.VMEM(*x) for x in shapes],
        in_specs=[pl.BlockSpec(memory_space=pltpu.HBM)] * 7,
        out_specs=[pl.BlockSpec(memory_space=vm)] * 5,
        scratch_shapes=scratch,
        compiler_params=pltpu.CompilerParams(
            collective_id=0, has_side_effects=True, vmem_limit_bytes=VMEM_BYTES - held - SPARE
        ),
    )(*arrays)
    query_grad, key_grad, value_grad, rot_grad, weight_grad = pl.pallas_call(
        put_out,
        out_shape=[jax.ShapeDtypeStruct(*x) for x in shapes],
        in_specs=[pl.BlockSpec(memory_space=vm)] * 5,
        out_specs=[pl.BlockSpec(memory_space=pltpu.HBM)] * 5,
        scratch_shapes=[dma(5)],
        compiler_params=pltpu.CompilerParams(vmem_limit_bytes=1 << 20),
    )(*results)
    return query_grad, key_grad, value_grad, rot_grad.T, weight_grad


def solution(mesh):
    placed = (
        P("sp", "tp"), P("sp", None), P("sp", None), P(None, "tp"),
        P("sp", "tp"), P("sp", "tp"), P("sp", "tp"),
    )
    return jax.shard_map(
        functools.partial(per_device, mesh.shape["sp"], mesh.shape["tp"]),
        mesh=mesh,
        in_specs=placed,
        out_specs=(P("sp", "tp"), P("sp", "tp"), P("sp", "tp"), P("sp", None), P("sp", "tp")),
        check_vma=False,
    )
```

```python
import functools
import math

import jax
import jax.numpy as jnp
from jax import lax
from jax.experimental import pallas as pl
from jax.experimental.pallas import tpu as pltpu
from jax.sharding import PartitionSpec as P

NOPE = 64
ROPE = 32
VDIM = 64
HEAD = NOPE + ROPE
VMEM_BYTES = 67043328
SPARE = 8192
MESH = pl.DeviceIdType.MESH
F32 = jnp.float32
BF16 = jnp.bfloat16


def dot(x, y, dims):
    return lax.dot_general(x, y, (dims, ((), ())), preferred_element_type=F32)


def three_terms(x):
    hi = x.astype(BF16)
    rest = x - hi.astype(F32)
    mid = rest.astype(BF16)
    low = (rest - mid.astype(F32)).astype(BF16)
    return hi, mid, low


def repeat(start, stop, body):
    if stop - start <= 4:
        for i in range(start, stop):
            body(i)
    else:
        def step(i, carry):
            body(i)
            return carry

        lax.fori_loop(start, stop, step, 0)


def kernel(
    S, TP, H,
    q_in, lat_in, rot_in, w_in, log_in, out_in, go_in,
    qg_ref, kg_ref, vg_ref, rg_ref, wg_ref,
    q_ref, lat_ref, rot_ref, w_ref, log_ref, out_ref, go_ref, loads, ps, pk, wq, kb, lb, ka_ref, va_ref, kat_ref, dk_acc, dv_acc, dq_own, dqs, dqr,
    kvo, kvr, ro, rr, rt, wgs, wgr, wh, wo, qo, qr,
    s1q, r1q, s1k, r1k, s1l, r1l, s2, r2, s3, r3, s4k, r4k, s4r, r4r, s4q, r4q, s5, r5, s6, r6, s7, r7, s8, r8,
):
    G = S // H
    T = q_ref.shape[0]
    half = T // 2
    me = lax.axis_index("sp")
    tpi = lax.axis_index("tp")
    a, b = me // G, lax.rem(me, G)
    scale = HEAD ** (-0.5)

    barrier = pltpu.get_barrier_semaphore()

    def greet(i):
        pl.semaphore_signal(barrier, inc=1, device_id={"sp": lax.rem(me + i, S)}, device_id_type=MESH)

    def greet_tp(i):
        pl.semaphore_signal(barrier, inc=1, device_id={"tp": lax.rem(tpi + i, TP)}, device_id_type=MESH)

    pairs = (
        (q_in, q_ref), (go_in, go_ref), (out_in, out_ref), (log_in, log_ref),
        (lat_in, lat_ref), (w_in, w_ref), (rot_in, rot_ref),
    )
    fetch = [pltpu.make_async_copy(x, y, loads.at[i]) for i, (x, y) in enumerate(pairs)]
    for f in fetch:
        f.start()
    repeat(1, S, greet)
    repeat(1, TP, greet_tp)

    def copy(src, dst, ssem, rsem, sp):
        return pltpu.make_async_remote_copy(
            src_ref=src, dst_ref=dst, send_sem=ssem, recv_sem=rsem,
            device_id={"sp": sp}, device_id_type=MESH,
        )

    for f in fetch[:4]:
        f.wait()
    logs_t = log_ref[...] * math.sqrt(HEAD)
    prod = out_ref[...].astype(F32) * go_ref[...].astype(F32)
    pad = jnp.zeros((T, ROPE - 6), BF16)
    for j in range(H):
        delta = jnp.sum(prod[:, VDIM * j : VDIM * (j + 1)], axis=1, keepdims=True)
        logs = jnp.broadcast_to(logs_t[j : j + 1], (8, T)).T[:, :1]
        terms = three_terms(logs) + three_terms(delta)
        ps[j, :T, :] = jnp.concatenate([q_ref[:, HEAD * j : HEAD * (j + 1)], *terms, pad], axis=1)
        g = go_ref[:, VDIM * j : VDIM * (j + 1)]
        ps[j, T:, :] = jnp.concatenate([g[:half], g[half:]], axis=1)
    wq[b, a] = ps[a]
    pl.semaphore_wait(barrier, S - 1 + TP - 1)

    firsts, lats = [], []
    for d in range(1, H):
        to = lax.rem(a + d, H)
        cq = copy(ps.at[to], wq.at[b, a], s1q.at[d - 1], r1q.at[d - 1], to * G + b)
        ck = copy(pk.at[to], kb.at[a], s1k.at[d - 1], r1k.at[d - 1], to * G + b)
        cq.start()
        firsts.append((cq, ck))

    def relay(d, e):
        src = wq.at[b, lax.rem(a - d + H, H)]
        return copy(src, src, s2.at[e - 1, d], r2.at[e - 1, d], a * G + lax.rem(b + e, G))

    def relay_all(d):
        repeat(1, G, lambda e: relay(d, e).start())

    relay_all(0)
    for f in fetch[4:]:
        f.wait()
    joined = dot(lat_ref[...], w_ref[...], ((1,), (0,))).astype(BF16)
    for j in range(H):
        pk[j, :T, :] = joined[:, 128 * j : 128 * (j + 1)]
        pk[j, T:, :] = rot_ref[...]
    kb[a] = pk[a]
    for d in range(1, H):
        firsts[d - 1][1].start()
    lb[a] = lat_ref[...].reshape(lb.shape[1:])
    slab = T // TP
    mine = lat_ref.at[pl.ds(pl.multiple_of(tpi * slab, slab), slab)]
    for d in range(1, H):
        to = lax.rem(a + d, H)
        cl = copy(mine, lb.at[a, tpi], s1l.at[d - 1], r1l.at[d - 1], to * G + b)
        cl.start()
        lats.append(cl)
    for d in range(1, H):
        firsts[d - 1][0].wait_recv()
        relay_all(d)
    for d in range(1, H):
        firsts[d - 1][1].wait_recv()

    lane = lax.broadcasted_iota(jnp.int32, (T, ROPE), 1)
    log_ones = jnp.where(lane < 3, -1.0, 0.0).astype(BF16)
    delta_ones = jnp.where((lane >= 3) & (lane < 6), -1.0, 0.0).astype(BF16)
    for j in range(H):
        kv = kb[j, :T, :]
        r = kb[j, T:, :].astype(F32).T.astype(BF16)
        key = jnp.concatenate([kv[:, :NOPE], r, log_ones], axis=1)
        ka_ref[T * j : T * (j + 1), :] = key
        va_ref[T * j : T * (j + 1), :128] = jnp.concatenate([jnp.zeros((T, HEAD), BF16), delta_ones], axis=1)
        va_ref[T * j : T * (j + 1), 128:] = jnp.concatenate([kv[:, NOPE:], jnp.zeros((T, 64), BF16)], axis=1)
        kat_ref[:, T * j : T * (j + 1)] = key.astype(F32).T.astype(BF16)[:HEAD]
    dk_acc[...] = jnp.zeros_like(dk_acc)
    dv_acc[...] = jnp.zeros_like(dv_acc)

    def block(e, keep):
        col = lax.rem(b - e + G, G)
        query = wq[col, :, :T, :].reshape(H * T, 128)
        gp = wq[col, :, T:, :]
        g = jnp.concatenate([gp[:, :, :VDIM], gp[:, :, VDIM:]], axis=1).reshape(H * T, VDIM)
        g = jnp.concatenate([g, jnp.zeros_like(g)], axis=1)
        s = dot(ka_ref[...], query, ((1,), (1,)))
        dp = dot(va_ref[...], jnp.concatenate([query, g], axis=1), ((1,), (1,)))
        p = jnp.exp(s * scale)
        ds = (p * dp).astype(BF16)
        keep(dot(kat_ref[...], ds, ((1,), (0,))) * scale)
        dv_acc[...] += dot(p.astype(BF16), g, ((1,), (0,)))
        dk_acc[...] += dot(ds, query, ((1,), (0,)))

    def part(e):
        return copy(dqs.at[e - 1], dqr.at[e - 1], s3.at[e - 1], r3.at[e - 1], a * G + lax.rem(b - e + G, G))

    def keep_own(x):
        dq_own[...] = x

    block(0, keep_own)

    def other(e):
        for d in range(H):
            relay(d, e).wait_recv()

        def send(x):
            dqs[e - 1] = x
            part(e).start()

        block(e, send)

    def hand_on(d, i):
        piece = lb.at[lax.rem(a - d + H, H), tpi]
        return pltpu.make_async_remote_copy(
            src_ref=piece, dst_ref=piece, send_sem=s8.at[d - 1, i - 1], recv_sem=r8.at[d - 1, i - 1],
            device_id={"tp": lax.rem(tpi + i, TP)}, device_id_type=MESH,
        )

    repeat(1, min(3, G), other)
    for d in range(1, H):
        lats[d - 1].wait_recv()
        repeat(1, TP, lambda i: hand_on(d, i).start())
    repeat(min(3, G), G, other)

    dk = dk_acc[...] * scale
    kv = jnp.concatenate([dk[:, :NOPE], dv_acc[:, :VDIM]], axis=1).astype(BF16)
    rot_t = dk.T[NOPE:HEAD]
    for j in range(H):
        kvo[j] = kv[T * j : T * (j + 1)]
        ro[j] = rot_t[:, T * j : T * (j + 1)]
    kvr[a] = kvo[a]
    rr[a] = ro[a]
    backs = []
    for d in range(1, H):
        to = lax.rem(a + d, H)
        ck = copy(kvo.at[to], kvr.at[a], s4k.at[d - 1], r4k.at[d - 1], to * G + b)
        cr = copy(ro.at[to], rr.at[a], s4r.at[d - 1], r4r.at[d - 1], to * G + b)
        cr.start()
        ck.start()
        backs += [ck, cr]

    for d in range(1, H):
        repeat(1, TP, lambda i: hand_on(d, i).wait_recv())
    lat = lb[...].reshape(H * T, lb.shape[3])
    total = dot(lat, kv, ((0,), (0,)))
    rows = wgs.shape[2]
    for i in range(G):
        for j in range(H):
            wgs[i, j] = total[(j * G + i) * rows : (j * G + i + 1) * rows]
    wgr[b] = wgs[b]

    def share(e):
        to = lax.rem(b + e, G)
        return copy(wgs.at[to], wgr.at[b], s5.at[e - 1], r5.at[e - 1], a * G + to)

    repeat(1, G, lambda e: share(e).start())

    def take(e):
        part(e).wait_recv()
        dq_own[...] += dqr[e - 1]

    repeat(1, G, take)
    dq = jnp.concatenate([dq_own[...], jnp.zeros((128 - HEAD, H * T), F32)], axis=0).T.astype(BF16)
    for j in range(H):
        qo[j] = dq[T * j : T * (j + 1)]
    qr[a] = qo[a]
    for d in range(1, H):
        to = lax.rem(a + d, H)
        cq = copy(qo.at[to], qr.at[a], s4q.at[d - 1], r4q.at[d - 1], to * G + b)
        cq.start()
        backs.append(cq)

    repeat(1, G, lambda e: share(e).wait_recv())
    wh[...] = functools.reduce(lambda x, y: x + y, [wgr[i] for i in range(G)])
    wo[a] = wh[a]
    lasts = []
    for d in range(1, H):
        to = lax.rem(a + d, H)
        c = copy(wh.at[to], wo.at[a], s7.at[d - 1], r7.at[d - 1], to * G + b)
        c.start()
        lasts.append(c)
    for d in range(1, H):
        backs[2 * (d - 1) + 1].wait_recv()
    rt[tpi] = functools.reduce(lambda x, y: x + y, [rr[j] for j in range(H)])

    def swap(i):
        return pltpu.make_async_remote_copy(
            src_ref=rt.at[tpi], dst_ref=rt.at[tpi], send_sem=s6.at[i - 1], recv_sem=r6.at[i - 1],
            device_id={"tp": lax.rem(tpi + i, TP)}, device_id_type=MESH,
        )

    repeat(1, TP, lambda i: swap(i).start())
    for d in range(1, H):
        backs[2 * (d - 1)].wait_recv()
    for j in range(H):
        kg_ref[:, NOPE * j : NOPE * (j + 1)] = kvr[j, :, :NOPE]
        vg_ref[:, VDIM * j : VDIM * (j + 1)] = kvr[j, :, NOPE:]
    repeat(1, TP, lambda i: swap(i).wait_recv())
    rot_sum = functools.reduce(lambda x, y: x + y, [rt[i] for i in range(TP)])
    rg_ref[...] = rot_sum
    for d in range(1, H):
        backs[2 * (H - 1) + d - 1].wait_recv()
    for j in range(H):
        qg_ref[:, HEAD * j : HEAD * (j + 1)] = qr[j, :, :HEAD]

    for c in lasts:
        c.wait_recv()
    for j in range(H):
        wg_ref[:, 128 * j : 128 * (j + 1)] = wo[j]

    for cq, ck in firsts:
        cq.wait_send()
        ck.wait_send()
    for c in lats + backs + lasts:
        c.wait_send()
    for d in range(H):
        repeat(1, G, lambda e: relay(d, e).wait_send())
    repeat(1, G, lambda e: part(e).wait_send())
    repeat(1, G, lambda e: share(e).wait_send())
    repeat(1, TP, lambda i: swap(i).wait_send())
    for d in range(1, H):
        repeat(1, TP, lambda i: hand_on(d, i).wait_send())


def put_out(*refs):
    copies = [pltpu.make_async_copy(refs[i], refs[5 + i], refs[10].at[i]) for i in range(5)]
    for c in copies:
        c.start()
    for c in copies:
        c.wait()


def per_device(S, TP, queries, latents, rot_key, kv_weight, log_sums, outputs, out_grad):
    T, rank = latents.shape
    H = log_sums.shape[1]
    G = S // H
    rows = rank // S
    wide = H * T
    dma = lambda *n: pltpu.SemaphoreType.DMA(tuple(max(k, 1) for k in n))
    pairs = lambda *n: [dma(*n), dma(*n)]
    vm = pltpu.VMEM
    g1 = max(G - 1, 1)
    arrays = (queries, latents, rot_key.T, kv_weight, log_sums.T, outputs, out_grad)
    scratch = [
        *[vm(x.shape, x.dtype) for x in arrays], dma(len(arrays)),
        vm((H, T + T // 2, 128), BF16), vm((H, T + ROPE, 128), BF16),
        vm((G, H, T + T // 2, 128), BF16), vm((H, T + ROPE, 128), BF16), vm((H, TP, T // TP, rank), BF16),
        vm((wide, 128), BF16), vm((wide, 256), BF16), vm((HEAD, wide), BF16),
        vm((wide, 128), F32), vm((wide, 128), F32), vm((HEAD, wide), F32),
        vm((g1, HEAD, wide), F32), vm((g1, HEAD, wide), F32),
        vm((H, T, 128), BF16), vm((H, T, 128), BF16), vm((H, ROPE, T), F32), vm((H, ROPE, T), F32),
        vm((TP, ROPE, T), F32), *[vm((G, H, rows, 128), F32)] * 2, *[vm((H, rows, 128), F32)] * 2,
        vm((H, T, 128), BF16), vm((H, T, 128), BF16),
        *pairs(H - 1), *pairs(H - 1), *pairs(H - 1), *pairs(G - 1, H), *pairs(G - 1),
        *pairs(H - 1), *pairs(H - 1), *pairs(H - 1), *pairs(G - 1), *pairs(TP - 1), *pairs(H - 1), *pairs(H - 1, TP - 1),
    ]
    shapes = [
        ((T, H * HEAD), BF16), ((T, H * NOPE), BF16), ((T, H * VDIM), BF16),
        ((ROPE, T), F32), ((rows, H * 128), F32),
    ]
    held = sum(x[0] * -(-x[1] // 128) * 128 * jnp.dtype(t).itemsize for x, t in shapes)
    results = pl.pallas_call(
        functools.partial(kernel, S, TP, H),
        out_shape=[pltpu.VMEM(*x) for x in shapes],
        in_specs=[pl.BlockSpec(memory_space=pltpu.HBM)] * 7,
        out_specs=[pl.BlockSpec(memory_space=vm)] * 5,
        scratch_shapes=scratch,
        compiler_params=pltpu.CompilerParams(
            collective_id=0, has_side_effects=True, vmem_limit_bytes=VMEM_BYTES - held - SPARE
        ),
    )(*arrays)
    query_grad, key_grad, value_grad, rot_grad, weight_grad = pl.pallas_call(
        put_out,
        out_shape=[jax.ShapeDtypeStruct(*x) for x in shapes],
        in_specs=[pl.BlockSpec(memory_space=vm)] * 5,
        out_specs=[pl.BlockSpec(memory_space=pltpu.HBM)] * 5,
        scratch_shapes=[dma(5)],
        compiler_params=pltpu.CompilerParams(vmem_limit_bytes=1 << 20),
    )(*results)
    return query_grad, key_grad, value_grad, rot_grad.T, weight_grad


def solution(mesh):
    placed = (
        P("sp", "tp"), P("sp", None), P("sp", None), P(None, "tp"),
        P("sp", "tp"), P("sp", "tp"), P("sp", "tp"),
    )
    return jax.shard_map(
        functools.partial(per_device, mesh.shape["sp"], mesh.shape["tp"]),
        mesh=mesh,
        in_specs=placed,
        out_specs=(P("sp", "tp"), P("sp", "tp"), P("sp", "tp"), P("sp", None), P("sp", "tp")),
        check_vma=False,
    )
```
